32 devices in a mesh: grp: 1, ep: 16 (over z, y, x), tp: 2 (over core).
Axes of the slice: x: 2, y: 2, z: 4, core: 2. Of those that a mesh axis runs over, the one named last changes fastest.
Arguments:
- tokens: bfloat16 [512, 2048], P(('grp', 'ep')), may hold values from -6 to 6
- in_gain: bfloat16 [2048], replicated, may hold values from 0.099609375 to 1.8984375
- route_expert: int32 [512, 6], P(('grp', 'ep')), may hold values from 0 to 15, all different within a row; in each aligned block of 32 rows (0 to 31, 32 to 63, ...) at most 16 rows name the same one
- route_weight: float32 [512, 6], P(('grp', 'ep')), may hold values from 0.05 to 1
- gate_weight: bfloat16 [16, 2048, 768], P('ep', None, 'tp'), may hold values from -0.125 to 0.125
- up_weight: bfloat16 [16, 2048, 768], P('ep', None, 'tp'), may hold values from -0.125 to 0.125
- down_weight: bfloat16 [16, 768, 2048], P('ep', 'tp'), may hold values from -1 to 1
- shared_gate: bfloat16 [2048, 768], P(None, 'tp'), may hold values from -0.125 to 0.125
- shared_up: bfloat16 [2048, 768], P(None, 'tp'), may hold values from -0.125 to 0.125
- shared_down: bfloat16 [768, 2048], P('tp'), may hold values from -1 to 1
- out_gain: bfloat16 [2048], P('tp'), may hold values from 0.099609375 to 1.8984375
Outputs:
- mixed: bfloat16 [512, 2048], P(('grp', 'ep'), 'tp')
The draws below stay inside these ranges and needn't reach their ends.
Inputs may be any that keep to these rules, and one draw needn't show every extreme that they name: `route_expert`: each row names 6 different experts. Among the rows of one device no expert is named more than 16 times, a bound that some block reaches.
All inputs are finite; a program needn't handle non-finite values.
Results may differ from the reference program's by a relative error of at most 0.0077.
Values may be sent and summed in bfloat16 or wider, within the bound.
A program may use at most 64 MiB of HBM per device.

```python
import math
import jax
import jax.numpy as jnp
import numpy as np
from jax import lax

D = 2048
FE = 768
FS = 768
TOPK = 6
TOK_DEV = 32
EXPERTS = 16
CAP = 16
TOKENS = 512
N_EP = 16
N_TP = 2


def down_matrix(key, fan_in, copies, columns):
    position = jnp.arange(columns, dtype=jnp.float32) / columns
    draws = jnp.clip(jax.random.normal(key, (copies, fan_in, columns), jnp.float32), -4.0, 4.0)
    factor = 0.5 * 3.0 ** position
    return draws * factor[None, None, :] * fan_in ** (-0.5)


def draw_down_weight(key, part):
    return down_matrix(jax.random.fold_in(key, 11), FE, EXPERTS, D).astype(jnp.bfloat16)


def draw_shared_down(key, part):
    return down_matrix(jax.random.fold_in(key, 23), FS, 1, D)[0].astype(jnp.bfloat16)


def block_scale(own_key, extent, cuts, low, top_value):
    loudness, own = 1.0, jax.random.fold_in(own_key, 6)
    for dim, shards_of in cuts:
        heights = jnp.exp(jax.random.uniform(jax.random.fold_in(own, dim), (shards_of,), jnp.float32, low / len(cuts), top_value / len(cuts)))
        loudness = loudness * jnp.repeat(heights, extent[dim] // shards_of).reshape([-1 if axis == dim else 1 for axis in range(len(extent))])
    return loudness


def shared_out(rng, own, number, rows, number_of, top, reach, skew):
    ranking = jax.random.permutation(rng, number_of)
    crowded, ordinary = portions_of(number_of, rows * top, reach, skew, True), portions_of(number_of, rows * top, reach, skew, False)
    places = jnp.arange(number_of)

    def named(lengths, offset_by):
        used = int((lengths > 0).sum())
        fixed = max(1, used // 4)
        moved = fixed + (places - fixed + offset_by * (used - fixed)) % max(1, number_of - fixed)
        return jnp.zeros((number_of,), jnp.int32).at[ranking[jnp.where(places < fixed, places, moved)]].set(jnp.asarray(lengths, jnp.int32))

    lengths = jnp.where(number % 4 == 0, named(crowded, number // 4), named(ordinary, number - number // 4 - 1))
    mixed = jax.random.permutation(jax.random.fold_in(own, 3), number_of)
    giver, receiver = mixed[0:number_of // 2 * 2:2], mixed[1:number_of // 2 * 2:2]
    slack = jnp.minimum(lengths[giver] - 1, reach - lengths[receiver]) // 2
    slack = jnp.where((giver == ranking[0]) | (receiver == ranking[0]) | (lengths[receiver] == 0), 0, jnp.maximum(slack, 0))
    moved = jax.random.randint(jax.random.fold_in(own, 4), (number_of // 2,), 0, 1 << 20) % (slack + 1)
    lengths = lengths.at[giver].add(-moved).at[receiver].add(moved)
    members = jnp.searchsorted(jnp.cumsum(lengths), jnp.arange(rows * top), side="right").astype(jnp.int32)
    grid = members.reshape(top, rows).T
    grid = grid[jax.random.permutation(jax.random.fold_in(own, 1), rows)]
    offset_by = jax.random.randint(jax.random.fold_in(own, 2), (rows, 1), 0, top)
    return jnp.take_along_axis(grid, (jnp.arange(top)[None, :] + offset_by) % top, axis=1)


def portions_of(amount, total, reach, lean, full):
    weights = [(1 << 20) // math.isqrt(grade ** lean) + 1 for grade in range(1, amount + 1)]
    largest = reach if full else min(reach, max(-(-total // amount), total * weights[0] // sum(weights)))
    least = 1 if total - largest >= amount - 1 else 0
    holding, rest = [largest] + [least] * (amount - 1), total - largest - least * (amount - 1)
    while rest > 0:
        free = [i for i in range(1, amount) if holding[i] < largest] or [i for i in range(1, amount) if holding[i] < reach]
        pool, left = sum([weights[i] for i in free]), rest
        for i in free:
            extra = min(reach - holding[i], max(1, left * weights[i] // pool), rest)
            holding[i] = holding[i] + extra
            rest = rest - extra
    return np.array(holding)


def scatter_about(key, shape, spread, reach, shards=(), kind=jnp.bfloat16):
    loudness = block_scale(key, shape, shards, -0.22, 0.18) if shards else 1.0
    array = jax.random.normal(key, shape, jnp.float32) * spread * loudness
    return jnp.minimum(jnp.maximum(array, -reach), reach).astype(kind)


def setup_inputs(seed: int = 0, part: int = 0) -> dict:
    keys = jax.random.split(jax.random.key(seed), 12)
    own_keys = jax.random.split(jax.random.fold_in(keys[11], part), 12)
    tokens = scatter_about(own_keys[0], (TOKENS, D), 1.0, 6.0, ((0, 16),))
    in_gain = jnp.clip(1.0 + 0.18 * jax.random.normal(keys[1], (D,), jnp.float32), 0.099609375, 1.8984375).astype(jnp.bfloat16)
    route_expert_keys = jax.random.split(jax.random.fold_in(own_keys[2], 1), TOKENS // TOK_DEV)
    route_expert_turns = jax.random.permutation(jax.random.fold_in(own_keys[2], 3), TOKENS // TOK_DEV)
    route_expert = jax.vmap(lambda own, number: shared_out(jax.random.fold_in(own_keys[2], 2), own, number, TOK_DEV, EXPERTS, TOPK, CAP, 2))(route_expert_keys, route_expert_turns).reshape((TOKENS, TOPK))
    route_weight = jnp.clip(jnp.exp(math.log(1.0) - 2.9957323 * jax.random.uniform(own_keys[3], (TOKENS, TOPK), jnp.float32) ** block_scale(own_keys[3], (TOKENS, TOPK), ((0, 16),), -0.2, 0.2)), 0.05, 1.0)
    gate_weight = scatter_about(keys[4], (EXPERTS, D, FE), D ** -0.5, 0.125, ((0, 16), (2, 2)))
    up_weight = scatter_about(keys[5], (EXPERTS, D, FE), D ** -0.5, 0.125, ((0, 16), (2, 2)))
    down_weight = draw_down_weight(jax.random.fold_in(keys[11], 71), part)
    shared_gate = scatter_about(keys[7], (D, FS), D ** -0.5, 0.125, ((1, 2),))
    shared_up = scatter_about(keys[8], (D, FS), D ** -0.5, 0.125, ((1, 2),))
    shared_down = draw_shared_down(jax.random.fold_in(keys[11], 71), part)
    out_gain = jnp.clip(1.0 + 0.18 * jax.random.normal(keys[10], (D,), jnp.float32), 0.099609375, 1.8984375).astype(jnp.bfloat16)
    return dict(tokens=tokens, in_gain=in_gain, route_expert=route_expert, route_weight=route_weight, gate_weight=gate_weight, up_weight=up_weight, down_weight=down_weight, shared_gate=shared_gate, shared_up=shared_up, shared_down=shared_down, out_gain=out_gain)


EPSILON = 1e-06

def normalize(values, gain_vector):
    floats = values.astype(jnp.float32)
    scaled = floats * lax.rsqrt(lax.optimization_barrier(jnp.mean(floats * floats, axis=-1, keepdims=True)) + EPSILON)
    return (scaled * gain_vector.astype(jnp.float32)).astype(jnp.bfloat16)

def swiglu_hidden(inputs, gate_here, up_here):
    gate_value = jnp.dot(inputs, gate_here, preferred_element_type=jnp.float32)
    upward = jnp.dot(inputs, up_here, preferred_element_type=jnp.float32)
    return (jax.nn.silu(gate_value) * upward).astype(jnp.bfloat16)

def split_product(hidden, down_here, pieces):
    inner_width = hidden.shape[1] // pieces
    running = jnp.zeros((hidden.shape[0], down_here.shape[1]), jnp.float32)
    for portion in range(pieces):
        partial_value = jnp.dot(hidden[:, portion * inner_width:(portion + 1) * inner_width], down_here[portion * inner_width:(portion + 1) * inner_width], preferred_element_type=jnp.float32)
        running = running + lax.optimization_barrier(partial_value.astype(jnp.bfloat16)).astype(jnp.float32)
    return running.astype(jnp.bfloat16)

def slot_tables(routes_here, experts, capacity):
    picked_count = routes_here.shape[0] * routes_here.shape[1]
    flattened = routes_here.reshape(picked_count).astype(jnp.int32)
    onehot = (flattened[:, None] == jnp.arange(experts, dtype=jnp.int32)[None, :]).astype(jnp.int32)
    earlier = (jnp.cumsum(onehot, axis=0) - onehot).astype(jnp.int32)
    ranked = lax.optimization_barrier(jnp.sum(earlier * onehot, axis=1)).astype(jnp.int32)
    slot_index = flattened * capacity + ranked
    source_token = jnp.arange(picked_count, dtype=jnp.int32) // routes_here.shape[1]
    matches = slot_index[None, :] == jnp.arange(experts * capacity, dtype=jnp.int32)[:, None]
    filled = jnp.any(matches, axis=1)
    slot_owner = lax.optimization_barrier(jnp.sum(jnp.where(matches, source_token[None, :], 0), axis=1)).astype(jnp.int32)
    return (slot_index, filled, slot_owner)

def reference(tokens, in_gain, route_expert, route_weight, gate_weight, up_weight, down_weight, shared_gate, shared_up, shared_down, out_gain):
    capacity = CAP
    normed = normalize(tokens, in_gain)
    grouped = route_expert.reshape(N_EP, TOK_DEV, TOPK)
    slot_index, filled, slot_owner = jax.vmap(lambda routes_here: slot_tables(routes_here, EXPERTS, capacity))(grouped)
    per_device = normed.reshape(N_EP, TOK_DEV, D)
    outgoing = jax.vmap(lambda rows_here, chosen, filled_here: jnp.where(filled_here[:, None], rows_here[chosen], jnp.zeros((), jnp.bfloat16)))(per_device, slot_owner, filled)
    by_expert = outgoing.reshape(N_EP, EXPERTS, capacity, D).transpose(1, 0, 2, 3).reshape(EXPERTS, N_EP * capacity, D)

    def expert_pass(inputs):
        expert_rows, gate_here, up_here, down_here = inputs
        return split_product(swiglu_hidden(expert_rows, gate_here, up_here), down_here, N_TP)
    results = lax.map(expert_pass, (by_expert, gate_weight, up_weight, down_weight))
    returned = results.reshape(EXPERTS, N_EP, capacity, D).transpose(1, 0, 2, 3).reshape(N_EP, EXPERTS * capacity, D)
    picked = jax.vmap(lambda result_rows, chosen: result_rows[chosen])(returned, slot_index).astype(jnp.float32)
    picked = picked * route_weight.reshape(N_EP, TOK_DEV * TOPK)[:, :, None]
    routed = lax.optimization_barrier(jnp.sum(picked.reshape(TOKENS, TOPK, D), axis=1))
    shared = split_product(swiglu_hidden(normed, shared_gate, shared_up), shared_down, N_TP).astype(jnp.float32)
    combined = shared + routed
    scaled = combined * lax.rsqrt(lax.optimization_barrier(jnp.mean(combined * combined, axis=1, keepdims=True)) + EPSILON)
    return (scaled * out_gain.astype(jnp.float32)).astype(jnp.bfloat16)
```

```python
import functools

import jax
import jax.numpy as jnp
from jax import lax
from jax.experimental import pallas as pl
from jax.experimental.pallas import tpu as pltpu
from jax.sharding import PartitionSpec as P

EPSILON = 1e-06
F32 = jnp.float32
BF16 = jnp.bfloat16


def dot(a, b):
    return jnp.dot(a, b, preferred_element_type=F32)


def dot_t(a, b):
    return lax.dot_general(a, b, (((1,), (1,)), ((), ())), preferred_element_type=F32)


def silu_product(gate_value, upward):
    return (gate_value * (1.0 / (1.0 + jnp.exp(-gate_value))) * upward).astype(BF16)


def kernel(
    outer,
    inner,
    cap,
    info_width,
    tokens,
    in_gain,
    route_expert,
    route_weight,
    out_gain,
    gate_hbm,
    up_hbm,
    down_hbm,
    sgate_hbm,
    sup_hbm,
    sdown_hbm,
    mixed,
    gate_w,
    up_w,
    down_w,
    sgate_w,
    sup_w,
    sdown_w,
    normed,
    column,
    staged,
    rows_in,
    gate_acc,
    up_acc,
    part_out,
    part_in,
    part_own,
    result,
    back,
    sum_out,
    sum_in,
    shared_out,
    shared_in,
    squares_out,
    squares_in,
    w_sem,
    col_send,
    col_recv,
    plane_send,
    plane_recv,
    pair_send,
    pair_recv,
    part_send,
    part_recv,
    shared_sem,
    back_send,
    back_recv,
    sum_send,
    sum_recv,
    sq_sem,
):
    ep = lax.axis_index("ep")
    tp = lax.axis_index("tp")
    z = ep // inner
    p = ep % inner
    other = 1 - tp
    experts = outer * inner
    local_tokens, width = tokens.shape
    half = width // 2

    loads = [
        pltpu.make_async_copy(src, dst, w_sem.at[i])
        for i, (src, dst) in enumerate(
            [
                (sgate_hbm, sgate_w),
                (sup_hbm, sup_w),
                (sdown_hbm, sdown_w),
                (gate_hbm.at[0], gate_w),
                (up_hbm.at[0], up_w),
                (down_hbm.at[0], down_w),
            ]
        )
    ]
    for load in loads:
        load.start()

    barrier = pltpu.get_barrier_semaphore()

    def greet(ep_to, tp_to):
        pl.semaphore_signal(
            barrier, inc=1, device_id={"ep": ep_to, "tp": tp_to}, device_id_type=pl.DeviceIdType.MESH
        )

    for d in range(1, outer):
        greet(lax.rem(z + d, outer) * inner + p, tp)
    for d in range(1, inner):
        greet(z * inner + lax.rem(p + d, inner), tp)
    greet(ep, other)

    def remote(src, dst, send, recv, ep_to, tp_to):
        return pltpu.make_async_remote_copy(
            src_ref=src,
            dst_ref=dst,
            send_sem=send,
            recv_sem=recv,
            device_id={"ep": ep_to, "tp": tp_to},
            device_id_type=pl.DeviceIdType.MESH,
        )

    floats = tokens[...].astype(F32)
    mean = jnp.sum(floats * floats, axis=1, keepdims=True) / width
    rows = (floats * lax.rsqrt(mean + EPSILON) * in_gain[...].astype(F32)).astype(BF16)
    normed[...] = rows

    lane = lax.broadcasted_iota(jnp.int32, (local_tokens, info_width), 1)
    lane_expert = lax.rem(lane, experts)
    named = jnp.zeros((local_tokens, info_width), F32)
    weight = jnp.zeros((local_tokens, info_width), F32)
    for k in range(route_expert.shape[1]):
        hit = route_expert[:, k : k + 1] == lane_expert
        named = named + jnp.where(hit, 1.0, 0.0)
        weight = weight + jnp.where(hit, route_weight[:, k : k + 1], 0.0)
    row_i = lax.broadcasted_iota(jnp.int32, (local_tokens, local_tokens), 0)
    col_i = lax.broadcasted_iota(jnp.int32, (local_tokens, local_tokens), 1)
    upto = jnp.where(col_i <= row_i, 1.0, 0.0).astype(BF16)
    place = dot(upto, named.astype(BF16)) * named
    high = weight.astype(BF16).astype(F32)
    info = jnp.where(lane < experts, place, jnp.where(lane < 2 * experts, high, weight - high))
    info = jnp.where(lane < 3 * experts, info, 0.0)

    @pl.when(tp == 0)
    def _():
        column[z, :, :half] = rows[:, :half]

    @pl.when(tp == 1)
    def _():
        column[z, :, :half] = rows[:, half:]

    column[z, :, half:] = info.astype(BF16)

    pl.semaphore_wait(barrier, outer + inner - 1)

    sends = []
    for d in range(1, outer):
        to = lax.rem(z + d, outer)
        copy = remote(
            column.at[z], column.at[z], col_send.at[to], col_recv.at[z], to * inner + p, tp
        )
        copy.start()
        sends.append(copy)

    slots = inner * cap
    slot_row = lax.broadcasted_iota(jnp.int32, (slots, info_width), 0)
    slot_lane = lax.broadcasted_iota(jnp.int32, (slots, info_width), 1)
    slot_expert = z * inner + slot_row // cap

    def selector(offset):
        return jnp.where(slot_lane == slot_expert + offset, 1.0, 0.0).astype(BF16)

    pick_place = selector(0)
    slot_rank = (lax.broadcasted_iota(jnp.int32, (slots, local_tokens), 0) % cap + 1).astype(F32)

    def dispatch(j):
        where = dot_t(pick_place, column[j, :, half:])
        onehot = jnp.where(where == slot_rank, 1.0, 0.0).astype(BF16)
        moved = dot(onehot, column[j, :, :half]).astype(BF16)
        staged[j] = moved.reshape(inner, cap, half)
        for d in range(1, inner):
            to = lax.rem(p + d, inner)
            copy = remote(
                staged.at[j, to],
                rows_in.at[tp, j, p],
                plane_send.at[j, to],
                plane_recv.at[j, p],
                z * inner + to,
                tp,
            )
            copy.start()
            sends.append(copy)
        rows_in[tp, j, p] = staged[j, p]

    dispatch(z)
    for d in range(1, outer):
        j = lax.rem(z + d, outer)
        remote(
            column.at[j], column.at[j], col_send.at[j], col_recv.at[j], ep, tp
        ).wait_recv()
        dispatch(j)

    for load in loads[:3]:
        load.wait()
    inputs = normed[...]
    shared_hidden = silu_product(dot(inputs, sgate_w[...]), dot(inputs, sup_w[...]))
    shared_out[...] = dot(
        shared_hidden, sdown_w[:, pl.ds(pl.multiple_of(other * half, half), half)]
    ).astype(BF16)
    shared_copy = remote(shared_out, shared_in, shared_sem.at[0], shared_sem.at[1], ep, other)
    shared_copy.start()
    shared_own = dot(shared_hidden, sdown_w[:, pl.ds(pl.multiple_of(tp * half, half), half)])

    for load in loads[3:]:
        load.wait()

    pair_copies = []
    for d in range(outer):
        j = lax.rem(z + d, outer)
        for e in range(1, inner):
            source = lax.rem(p + e, inner)
            remote(
                staged.at[j, source],
                rows_in.at[tp, j, source],
                plane_send.at[j, source],
                plane_recv.at[j, source],
                ep,
                tp,
            ).wait_recv()
        copy = remote(
            rows_in.at[tp, j], rows_in.at[tp, j], pair_send.at[j], pair_recv.at[j], ep, other
        )
        copy.start()
        pair_copies.append(copy)

    total = experts * cap

    def half_rows(which):
        return pl.ds(pl.multiple_of(which * half, half), half)

    own_rows = rows_in[tp].reshape(total, half)
    gate_acc[...] = dot(own_rows, gate_w[half_rows(tp), :])
    up_acc[...] = dot(own_rows, up_w[half_rows(tp), :])
    for d in range(outer):
        j = lax.rem(z + d, outer)
        remote(
            rows_in.at[other, j], rows_in.at[other, j], pair_send.at[j], pair_recv.at[j], ep, other
        ).wait_recv()
    other_rows = rows_in[other].reshape(total, half)
    gate_value = gate_acc[...] + dot(other_rows, gate_w[half_rows(other), :])
    upward = up_acc[...] + dot(other_rows, up_w[half_rows(other), :])
    hidden = silu_product(gate_value, upward)

    part_out[...] = (
        dot(hidden, down_w[:, half_rows(other)]).astype(BF16).reshape(outer, inner, cap, half)
    )
    for d in range(outer):
        j = lax.rem(z + 1 + d, outer)
        copy = remote(part_out.at[j], part_in.at[j], part_send.at[j], part_recv.at[j], ep, other)
        copy.start()
        sends.append(copy)
    part_own[...] = (
        dot(hidden, down_w[:, half_rows(tp)]).astype(BF16).reshape(outer, inner, cap, half)
    )

    for d in range(outer):
        j = lax.rem(z + 1 + d, outer)
        remote(
            part_out.at[j], part_in.at[j], part_send.at[j], part_recv.at[j], ep, other
        ).wait_recv()
        summed = part_own[j].astype(F32) + part_in[j].astype(F32)
        result[j] = summed.astype(BF16)
        for e in range(1, inner):
            to = lax.rem(p + e, inner)
            copy = remote(
                result.at[j, to],
                back.at[j, p],
                back_send.at[j, to],
                back_recv.at[j, p],
                z * inner + to,
                tp,
            )
            copy.start()
            sends.append(copy)
        back[j, p] = result[j, p]

    pick_high = selector(experts)
    pick_low = selector(2 * experts)
    slot_of_lane = (lax.broadcasted_iota(jnp.int32, (local_tokens, slots), 1) % cap + 1).astype(F32)

    def combine(j):
        facts = column[j, :, half:]
        chosen = dot_t(facts, pick_place) == slot_of_lane
        high_part = jnp.where(chosen, dot_t(facts, pick_high), 0.0).astype(BF16)
        low_part = jnp.where(chosen, dot_t(facts, pick_low), 0.0).astype(BF16)
        for e in range(1, inner):
            source = lax.rem(p + e, inner)
            remote(
                result.at[j, source],
                back.at[j, source],
                back_send.at[j, source],
                back_recv.at[j, source],
                ep,
                tp,
            ).wait_recv()
        values = back[j].reshape(slots, half)
        return dot(high_part, values) + dot(low_part, values)

    for d in range(1, outer):
        j = lax.rem(z + d, outer)
        sum_out[j] = combine(j).astype(BF16)
        copy = remote(
            sum_out.at[j], sum_in.at[z], sum_send.at[j], sum_recv.at[z], j * inner + p, tp
        )
        copy.start()
        sends.append(copy)
    combined = combine(z)
    shared_copy.wait_recv()
    combined = combined + (
        shared_own.astype(BF16).astype(F32) + shared_in[...].astype(F32)
    ).astype(BF16).astype(F32)
    for d in range(1, outer):
        j = lax.rem(z + d, outer)
        remote(
            sum_out.at[j], sum_in.at[j], sum_send.at[j], sum_recv.at[j], ep, tp
        ).wait_recv()
        combined = combined + sum_in[j].astype(F32)

    own_squares = jnp.sum(combined * combined, axis=1, keepdims=True)
    squares_out[...] = jnp.broadcast_to(own_squares, squares_out.shape)
    sq_copy = remote(squares_out, squares_in, sq_sem.at[0], sq_sem.at[1], ep, other)
    sq_copy.start()
    sq_copy.wait_recv()
    squares = own_squares + squares_in[:, :1]
    scaled = combined * lax.rsqrt(squares / width + EPSILON)
    mixed[...] = (scaled * out_gain[...].astype(F32)).astype(BF16)

    for copy in sends:
        copy.wait_send()
    for copy in pair_copies:
        copy.wait_send()
    shared_copy.wait_send()
    sq_copy.wait_send()


def body(
    experts,
    tokens,
    in_gain,
    route_expert,
    route_weight,
    gate_weight,
    up_weight,
    down_weight,
    shared_gate,
    shared_up,
    shared_down,
    out_gain,
):
    inner = 1
    while inner * inner < experts:
        inner *= 2
    outer = experts // inner
    local_tokens, width = tokens.shape
    half = width // 2
    top_count = route_expert.shape[1]
    capacity = max(2, (local_tokens * top_count * 4 + 3 * experts - 1) // (3 * experts))
    cap = -(-capacity // 16) * 16
    info_width = -(-3 * experts // 128) * 128
    hidden = gate_weight.shape[2]
    shared_width = shared_gate.shape[1]
    total = experts * cap

    def vm(shape, kind=BF16):
        return pltpu.VMEM(shape, kind)

    grid_rows = (outer, inner, cap, half)
    dma = pltpu.SemaphoreType.DMA
    in_vmem = pl.BlockSpec(memory_space=pltpu.VMEM)
    anywhere = pl.BlockSpec(memory_space=pl.ANY)
    return pl.pallas_call(
        functools.partial(kernel, outer, inner, cap, info_width),
        out_shape=jax.ShapeDtypeStruct((local_tokens, half), BF16),
        in_specs=[in_vmem] * 5 + [anywhere] * 6,
        out_specs=in_vmem,
        scratch_shapes=[
            vm((width, hidden)),
            vm((width, hidden)),
            vm((hidden, width)),
            vm((width, shared_width)),
            vm((width, shared_width)),
            vm((shared_width, width)),
            vm((local_tokens, width)),
            vm((outer, local_tokens, half + info_width)),
            vm(grid_rows),
            vm((2,) + grid_rows),
            vm((total, hidden), F32),
            vm((total, hidden), F32),
            vm(grid_rows),
            vm(grid_rows),
            vm(grid_rows),
            vm(grid_rows),
            vm(grid_rows),
            vm((outer, local_tokens, half)),
            vm((outer, local_tokens, half)),
            vm((local_tokens, half)),
            vm((local_tokens, half)),
            vm((local_tokens, 128), F32),
            vm((local_tokens, 128), F32),
            dma((6,)),
            dma((outer,)),
            dma((outer,)),
            dma((outer, inner)),
            dma((outer, inner)),
            dma((outer,)),
            dma((outer,)),
            dma((outer,)),
            dma((outer,)),
            dma((2,)),
            dma((outer, inner)),
            dma((outer, inner)),
            dma((outer,)),
            dma((outer,)),
            dma((2,)),
        ],
        compiler_params=pltpu.CompilerParams(
            collective_id=0, has_side_effects=True, vmem_limit_bytes=60 * 1024 * 1024
        ),
    )(
        tokens,
        in_gain.reshape(1, width),
        route_expert,
        route_weight,
        out_gain.reshape(1, half),
        gate_weight,
        up_weight,
        down_weight,
        shared_gate,
        shared_up,
        shared_down,
    )


def solution(mesh):
    return jax.shard_map(
        functools.partial(body, mesh.shape["ep"]),
        mesh=mesh,
        in_specs=(
            P(("grp", "ep"), None),
            P(),
            P(("grp", "ep"), None),
            P(("grp", "ep"), None),
            P("ep", None, "tp"),
            P("ep", None, "tp"),
            P("ep", "tp", None),
            P(None, "tp"),
            P(None, "tp"),
            P("tp", None),
            P("tp"),
        ),
        out_specs=P(("grp", "ep"), "tp"),
        check_vma=False,
    )
```

```python
import functools

import jax
import jax.numpy as jnp
from jax import lax
from jax.experimental import pallas as pl
from jax.experimental.pallas import tpu as pltpu
from jax.sharding import PartitionSpec as P

EPSILON = 1e-06
F32 = jnp.float32
BF16 = jnp.bfloat16


def dot(a, b):
    return jnp.dot(a, b, preferred_element_type=F32)


def dot_t(a, b):
    return lax.dot_general(a, b, (((1,), (1,)), ((), ())), preferred_element_type=F32)


def silu_product(gate_value, upward):
    return (gate_value * (1.0 / (1.0 + jnp.exp(-gate_value))) * upward).astype(BF16)


def kernel(
    outer,
    inner,
    cap,
    info_width,
    tokens,
    in_gain,
    route_expert,
    route_weight,
    out_gain,
    gate_hbm,
    up_hbm,
    down_hbm,
    sgate_hbm,
    sup_hbm,
    sdown_hbm,
    mixed,
    gate_w,
    up_w,
    down_w,
    sgate_w,
    sup_w,
    sdown_w,
    normed,
    column,
    staged,
    rows_in,
    gate_acc,
    up_acc,
    part_out,
    part_in,
    part_own,
    result,
    back,
    sum_out,
    sum_in,
    shared_out,
    shared_in,
    squares_out,
    squares_in,
    w_sem,
    col_send,
    col_recv,
    plane_send,
    plane_recv,
    pair_send,
    pair_recv,
    part_send,
    part_recv,
    shared_sem,
    back_send,
    back_recv,
    sum_send,
    sum_recv,
    sq_sem,
):
    ep = lax.axis_index("ep")
    tp = lax.axis_index("tp")
    z = ep // inner
    p = ep % inner
    other = 1 - tp
    experts = outer * inner
    local_tokens, width = tokens.shape
    half = width // 2

    loads = [
        pltpu.make_async_copy(src, dst, w_sem.at[i])
        for i, (src, dst) in enumerate(
            [
                (sgate_hbm, sgate_w),
                (sup_hbm, sup_w),
                (sdown_hbm, sdown_w),
                (gate_hbm.at[0], gate_w),
                (up_hbm.at[0], up_w),
                (down_hbm.at[0], down_w),
            ]
        )
    ]
    for load in loads:
        load.start()

    barrier = pltpu.get_barrier_semaphore()

    def greet(ep_to, tp_to):
        pl.semaphore_signal(
            barrier, inc=1, device_id={"ep": ep_to, "tp": tp_to}, device_id_type=pl.DeviceIdType.MESH
        )

    for d in range(1, outer):
        greet(lax.rem(z + d, outer) * inner + p, tp)
    for d in range(1, inner):
        greet(z * inner + lax.rem(p + d, inner), tp)
    greet(ep, other)

    def remote(src, dst, send, recv, ep_to, tp_to):
        return pltpu.make_async_remote_copy(
            src_ref=src,
            dst_ref=dst,
            send_sem=send,
            recv_sem=recv,
            device_id={"ep": ep_to, "tp": tp_to},
            device_id_type=pl.DeviceIdType.MESH,
        )

    floats = tokens[...].astype(F32)
    mean = jnp.sum(floats * floats, axis=1, keepdims=True) / width
    rows = (floats * lax.rsqrt(mean + EPSILON) * in_gain[...].astype(F32)[None, :]).astype(BF16)
    normed[...] = rows

    fact = lax.broadcasted_iota(jnp.int32, (info_width, local_tokens), 0)
    fact_expert = lax.rem(fact, experts)
    named = jnp.zeros((info_width, local_tokens), F32)
    weight = jnp.zeros((info_width, local_tokens), F32)
    for k in range(route_expert.shape[0]):
        hit = route_expert[k : k + 1, :] == fact_expert
        named = named + jnp.where(hit, 1.0, 0.0)
        weight = weight + jnp.where(hit, route_weight[k : k + 1, :], 0.0)
    row_i = lax.broadcasted_iota(jnp.int32, (local_tokens, local_tokens), 0)
    col_i = lax.broadcasted_iota(jnp.int32, (local_tokens, local_tokens), 1)
    upto = jnp.where(row_i <= col_i, 1.0, 0.0).astype(BF16)
    place = dot(named.astype(BF16), upto) * named
    high = weight.astype(BF16).astype(F32)
    facts = jnp.where(fact < experts, place, jnp.where(fact < 2 * experts, high, weight - high))
    facts = jnp.where(fact < 3 * experts, facts, 0.0).astype(BF16)
    same = jnp.where(row_i == col_i, 1.0, 0.0).astype(BF16)
    info = dot_t(same, facts)

    @pl.when(tp == 0)
    def _():
        column[z, :, :half] = rows[:, :half]

    @pl.when(tp == 1)
    def _():
        column[z, :, :half] = rows[:, half:]

    column[z, :, half:] = info.astype(BF16)

    pl.semaphore_wait(barrier, outer + inner - 1)

    sends = []
    for d in range(1, outer):
        to = lax.rem(z + d, outer)
        copy = remote(
            column.at[z], column.at[z], col_send.at[to], col_recv.at[z], to * inner + p, tp
        )
        copy.start()
        sends.append(copy)

    slots = inner * cap
    slot_row = lax.broadcasted_iota(jnp.int32, (slots, info_width), 0)
    slot_lane = lax.broadcasted_iota(jnp.int32, (slots, info_width), 1)
    slot_expert = z * inner + slot_row // cap

    def selector(offset):
        return jnp.where(slot_lane == slot_expert + offset, 1.0, 0.0).astype(BF16)

    pick_place = selector(0)
    slot_rank = (lax.broadcasted_iota(jnp.int32, (slots, local_tokens), 0) % cap + 1).astype(F32)

    def dispatch(j):
        where = dot_t(pick_place, column[j, :, half:])
        onehot = jnp.where(where == slot_rank, 1.0, 0.0).astype(BF16)
        moved = dot(onehot, column[j, :, :half]).astype(BF16)
        staged[j] = moved.reshape(inner, cap, half)
        for d in range(1, inner):
            to = lax.rem(p + d, inner)
            copy = remote(
                staged.at[j, to],
                rows_in.at[tp, j, p],
                plane_send.at[j, to],
                plane_recv.at[j, p],
                z * inner + to,
                tp,
            )
            copy.start()
            sends.append(copy)
        rows_in[tp, j, p] = staged[j, p]

    dispatch(z)

    for load in loads[:3]:
        load.wait()
    inputs = normed[...]
    shared_hidden = silu_product(dot(inputs, sgate_w[...]), dot(inputs, sup_w[...]))
    shared_out[...] = dot(
        shared_hidden, sdown_w[:, pl.ds(pl.multiple_of(other * half, half), half)]
    ).astype(BF16)
    shared_copy = remote(shared_out, shared_in, shared_sem.at[0], shared_sem.at[1], ep, other)
    shared_copy.start()
    shared_own = dot(shared_hidden, sdown_w[:, pl.ds(pl.multiple_of(tp * half, half), half)])

    for d in range(1, outer):
        j = lax.rem(z + d, outer)
        remote(
            column.at[j], column.at[j], col_send.at[j], col_recv.at[j], ep, tp
        ).wait_recv()
        dispatch(j)

    for load in loads[3:]:
        load.wait()

    pair_copies = []
    for d in range(outer):
        j = lax.rem(z + d, outer)
        for e in range(1, inner):
            source = lax.rem(p + e, inner)
            remote(
                staged.at[j, source],
                rows_in.at[tp, j, source],
                plane_send.at[j, source],
                plane_recv.at[j, source],
                ep,
                tp,
            ).wait_recv()
        copy = remote(
            rows_in.at[tp, j], rows_in.at[tp, j], pair_send.at[j], pair_recv.at[j], ep, other
        )
        copy.start()
        pair_copies.append(copy)

    total = experts * cap

    def half_rows(which):
        return pl.ds(pl.multiple_of(which * half, half), half)

    own_rows = rows_in[tp].reshape(total, half)
    gate_acc[...] = dot(own_rows, gate_w[half_rows(tp), :])
    up_acc[...] = dot(own_rows, up_w[half_rows(tp), :])
    for d in range(outer):
        j = lax.rem(z + d, outer)
        remote(
            rows_in.at[other, j], rows_in.at[other, j], pair_send.at[j], pair_recv.at[j], ep, other
        ).wait_recv()
    other_rows = rows_in[other].reshape(total, half)
    gate_value = gate_acc[...] + dot(other_rows, gate_w[half_rows(other), :])
    upward = up_acc[...] + dot(other_rows, up_w[half_rows(other), :])
    hidden = silu_product(gate_value, upward)

    part_out[...] = (
        dot(hidden, down_w[:, half_rows(other)]).astype(BF16).reshape(outer, inner, cap, half)
    )
    for d in range(outer):
        j = lax.rem(z + 1 + d, outer)
        copy = remote(part_out.at[j], part_in.at[j], part_send.at[j], part_recv.at[j], ep, other)
        copy.start()
        sends.append(copy)
    part_own[...] = (
        dot(hidden, down_w[:, half_rows(tp)]).astype(BF16).reshape(outer, inner, cap, half)
    )

    for d in range(outer):
        j = lax.rem(z + 1 + d, outer)
        remote(
            part_out.at[j], part_in.at[j], part_send.at[j], part_recv.at[j], ep, other
        ).wait_recv()
        summed = part_own[j].astype(F32) + part_in[j].astype(F32)
        result[j] = summed.astype(BF16)
        for e in range(1, inner):
            to = lax.rem(p + e, inner)
            copy = remote(
                result.at[j, to],
                back.at[j, p],
                back_send.at[j, to],
                back_recv.at[j, p],
                z * inner + to,
                tp,
            )
            copy.start()
            sends.append(copy)
        back[j, p] = result[j, p]

    pick_high = selector(experts)
    pick_low = selector(2 * experts)
    slot_of_lane = (lax.broadcasted_iota(jnp.int32, (local_tokens, slots), 1) % cap + 1).astype(F32)

    def combine(j):
        facts = column[j, :, half:]
        chosen = dot_t(facts, pick_place) == slot_of_lane
        high_part = jnp.where(chosen, dot_t(facts, pick_high), 0.0).astype(BF16)
        low_part = jnp.where(chosen, dot_t(facts, pick_low), 0.0).astype(BF16)
        for e in range(1, inner):
            source = lax.rem(p + e, inner)
            remote(
                result.at[j, source],
                back.at[j, source],
                back_send.at[j, source],
                back_recv.at[j, source],
                ep,
                tp,
            ).wait_recv()
        values = back[j].reshape(slots, half)
        return dot(high_part, values) + dot(low_part, values)

    for d in range(1, outer):
        j = lax.rem(z + d, outer)
        sum_out[j] = combine(j).astype(BF16)
        copy = remote(
            sum_out.at[j], sum_in.at[z], sum_send.at[j], sum_recv.at[z], j * inner + p, tp
        )
        copy.start()
        sends.append(copy)
    combined = combine(z)
    shared_copy.wait_recv()
    combined = combined + (
        shared_own.astype(BF16).astype(F32) + shared_in[...].astype(F32)
    ).astype(BF16).astype(F32)
    for d in range(1, outer):
        j = lax.rem(z + d, outer)
        remote(
            sum_out.at[j], sum_in.at[j], sum_send.at[j], sum_recv.at[j], ep, tp
        ).wait_recv()
        combined = combined + sum_in[j].astype(F32)

    own_squares = jnp.sum(combined * combined, axis=1, keepdims=True)
    squares_out[...] = jnp.broadcast_to(own_squares, squares_out.shape)
    sq_copy = remote(squares_out, squares_in, sq_sem.at[0], sq_sem.at[1], ep, other)
    sq_copy.start()
    sq_copy.wait_recv()
    squares = own_squares + squares_in[:, :1]
    scaled = combined * lax.rsqrt(squares / width + EPSILON)
    mixed[...] = (scaled * out_gain[...].astype(F32)[None, :]).astype(BF16)

    for copy in sends:
        copy.wait_send()
    for copy in pair_copies:
        copy.wait_send()
    shared_copy.wait_send()
    sq_copy.wait_send()


def body(
    experts,
    tokens,
    in_gain,
    route_expert,
    route_weight,
    gate_weight,
    up_weight,
    down_weight,
    shared_gate,
    shared_up,
    shared_down,
    out_gain,
):
    inner = 1
    while inner * inner < experts:
        inner *= 2
    outer = experts // inner
    local_tokens, width = tokens.shape
    half = width // 2
    top_count = route_expert.shape[1]
    capacity = max(2, (local_tokens * top_count * 4 + 3 * experts - 1) // (3 * experts))
    cap = -(-capacity // 16) * 16
    info_width = -(-3 * experts // 128) * 128
    hidden = gate_weight.shape[2]
    shared_width = shared_gate.shape[1]
    total = experts * cap

    def vm(shape, kind=BF16):
        return pltpu.VMEM(shape, kind)

    grid_rows = (outer, inner, cap, half)
    dma = pltpu.SemaphoreType.DMA
    in_vmem = pl.BlockSpec(memory_space=pltpu.VMEM)
    anywhere = pl.BlockSpec(memory_space=pl.ANY)
    return pl.pallas_call(
        functools.partial(kernel, outer, inner, cap, info_width),
        out_shape=jax.ShapeDtypeStruct((local_tokens, half), BF16),
        in_specs=[in_vmem] * 5 + [anywhere] * 6,
        out_specs=in_vmem,
        scratch_shapes=[
            vm((width, hidden)),
            vm((width, hidden)),
            vm((hidden, width)),
            vm((width, shared_width)),
            vm((width, shared_width)),
            vm((shared_width, width)),
            vm((local_tokens, width)),
            vm((outer, local_tokens, half + info_width)),
            vm(grid_rows),
            vm((2,) + grid_rows),
            vm((total, hidden), F32),
            vm((total, hidden), F32),
            vm(grid_rows),
            vm(grid_rows),
            vm(grid_rows),
            vm(grid_rows),
            vm(grid_rows),
            vm((outer, local_tokens, half)),
            vm((outer, local_tokens, half)),
            vm((local_tokens, half)),
            vm((local_tokens, half)),
            vm((local_tokens, 128), F32),
            vm((local_tokens, 128), F32),
            dma((6,)),
            dma((outer,)),
            dma((outer,)),
            dma((outer, inner)),
            dma((outer, inner)),
            dma((outer,)),
            dma((outer,)),
            dma((outer,)),
            dma((outer,)),
            dma((2,)),
            dma((outer, inner)),
            dma((outer, inner)),
            dma((outer,)),
            dma((outer,)),
            dma((2,)),
        ],
        compiler_params=pltpu.CompilerParams(
            collective_id=0, has_side_effects=True, vmem_limit_bytes=60 * 1024 * 1024
        ),
    )(
        tokens,
        in_gain,
        route_expert.T,
        route_weight.T,
        out_gain,
        gate_weight,
        up_weight,
        down_weight,
        shared_gate,
        shared_up,
        shared_down,
    )


def solution(mesh):
    return jax.shard_map(
        functools.partial(body, mesh.shape["ep"]),
        mesh=mesh,
        in_specs=(
            P(("grp", "ep"), None),
            P(),
            P(("grp", "ep"), None),
            P(("grp", "ep"), None),
            P("ep", None, "tp"),
            P("ep", None, "tp"),
            P("ep", "tp", None),
            P(None, "tp"),
            P(None, "tp"),
            P("tp", None),
            P("tp"),
        ),
        out_specs=P(("grp", "ep"), "tp"),
        check_vma=False,
    )
```

```python
import functools

import jax
import jax.numpy as jnp
from jax import lax
from jax.experimental import pallas as pl
from jax.experimental.pallas import tpu as pltpu
from jax.sharding import PartitionSpec as P

EPSILON = 1e-06
F32 = jnp.float32
BF16 = jnp.bfloat16


def dot(a, b):
    return jnp.dot(a, b, preferred_element_type=F32)


def dot_t(a, b):
    return lax.dot_general(a, b, (((1,), (1,)), ((), ())), preferred_element_type=F32)


def silu_product(gate_value, upward):
    return (gate_value * (1.0 / (1.0 + jnp.exp(-gate_value))) * upward).astype(BF16)


def kernel(
    outer,
    inner,
    cap,
    info_width,
    tokens,
    in_gain,
    route_expert,
    route_weight,
    out_gain,
    gate_hbm,
    up_hbm,
    down_hbm,
    sgate_hbm,
    sup_hbm,
    sdown_hbm,
    mixed,
    gate_w,
    up_w,
    down_w,
    sgate_w,
    sup_w,
    sdown_w,
    normed,
    column,
    staged,
    rows_in,
    part_out,
    part_in,
    part_own,
    result,
    back,
    sum_out,
    sum_in,
    shared_out,
    shared_in,
    squares_out,
    squares_in,
    w_sem,
    col_send,
    col_recv,
    col_pass,
    plane_send,
    plane_recv,
    pair_send,
    pair_recv,
    part_send,
    part_recv,
    shared_sem,
    back_send,
    back_recv,
    sum_send,
    sum_recv,
    sq_sem,
):
    ep = lax.axis_index("ep")
    tp = lax.axis_index("tp")
    z = ep // inner
    p = ep % inner
    other = 1 - tp
    experts = outer * inner
    local_tokens, width = tokens.shape
    half = width // 2

    loads = [
        pltpu.make_async_copy(src, dst, w_sem.at[i])
        for i, (src, dst) in enumerate(
            [
                (sgate_hbm, sgate_w),
                (sup_hbm, sup_w),
                (sdown_hbm, sdown_w),
                (gate_hbm.at[0], gate_w),
                (up_hbm.at[0], up_w),
                (down_hbm.at[0], down_w),
            ]
        )
    ]
    for load in loads:
        load.start()

    barrier = pltpu.get_barrier_semaphore()

    def greet(ep_to, tp_to):
        pl.semaphore_signal(
            barrier, inc=1, device_id={"ep": ep_to, "tp": tp_to}, device_id_type=pl.DeviceIdType.MESH
        )

    for d in range(1, outer):
        greet(lax.rem(z + d, outer) * inner + p, tp)
    for d in range(1, inner):
        greet(z * inner + lax.rem(p + d, inner), tp)
    greet(ep, other)

    def remote(src, dst, send, recv, ep_to, tp_to):
        return pltpu.make_async_remote_copy(
            src_ref=src,
            dst_ref=dst,
            send_sem=send,
            recv_sem=recv,
            device_id={"ep": ep_to, "tp": tp_to},
            device_id_type=pl.DeviceIdType.MESH,
        )

    floats = tokens[...].astype(F32)
    mean = jnp.sum(floats * floats, axis=1, keepdims=True) / width
    rows = (floats * lax.rsqrt(mean + EPSILON) * in_gain[...].astype(F32)[None, :]).astype(BF16)
    normed[...] = rows

    fact = lax.broadcasted_iota(jnp.int32, (info_width, local_tokens), 0)
    fact_expert = lax.rem(fact, experts)
    named = jnp.zeros((info_width, local_tokens), F32)
    weight = jnp.zeros((info_width, local_tokens), F32)
    for k in range(route_expert.shape[0]):
        hit = route_expert[k : k + 1, :] == fact_expert
        named = named + jnp.where(hit, 1.0, 0.0)
        weight = weight + jnp.where(hit, route_weight[k : k + 1, :], 0.0)
    row_i = lax.broadcasted_iota(jnp.int32, (local_tokens, local_tokens), 0)
    col_i = lax.broadcasted_iota(jnp.int32, (local_tokens, local_tokens), 1)
    upto = jnp.where(row_i <= col_i, 1.0, 0.0).astype(BF16)
    place = dot(named.astype(BF16), upto) * named
    high = weight.astype(BF16).astype(F32)
    facts = jnp.where(fact < experts, place, jnp.where(fact < 2 * experts, high, weight - high))
    facts = jnp.where(fact < 3 * experts, facts, 0.0).astype(BF16)
    same = jnp.where(row_i == col_i, 1.0, 0.0).astype(BF16)
    info = dot_t(same, facts)

    @pl.when(tp == 0)
    def _():
        column[z, :, :half] = rows[:, :half]

    @pl.when(tp == 1)
    def _():
        column[z, :, :half] = rows[:, half:]

    column[z, :, half:] = info.astype(BF16)

    pl.semaphore_wait(barrier, outer + inner - 1)

    sends = []

    def send(src, dst, send_sem, recv_sem, ep_to, tp_to):
        copy = remote(src, dst, send_sem, recv_sem, ep_to, tp_to)
        copy.start()
        sends.append(copy)

    def arrive(ref, send_sem, recv_sem):
        remote(ref, ref, send_sem, recv_sem, ep, other).wait_recv()

    short = jnp.minimum(z, outer - 1 - z)

    def nth(i):
        if i == 0:
            return z
        near = (i + 1) // 2 if i % 2 else -(i // 2)
        far = jnp.where(z < outer - 1 - z, i - short, short - i)
        return z + jnp.where(i <= 2 * short, near, far)

    order = [nth(i) for i in range(outer)]

    def column_copy(block, to, send_sem):
        here = column.at[block]
        return remote(here, here, send_sem, col_recv.at[block], to * inner + p, tp)

    def direct(to):
        return (to - z) * (to - z) != 4

    def passes(j):
        on = 2 * z - j
        return on, ((j - z) * (j - z) == 1) & (on >= 0) & (on < outer)

    for to in order[1:]:

        @pl.when(direct(to))
        def _(to=to):
            column_copy(z, to, col_send.at[to]).start()


    slots = inner * cap
    slot_row = lax.broadcasted_iota(jnp.int32, (slots, info_width), 0)
    slot_lane = lax.broadcasted_iota(jnp.int32, (slots, info_width), 1)
    slot_expert = z * inner + slot_row // cap

    def selector(offset):
        return jnp.where(slot_lane == slot_expert + offset, 1.0, 0.0).astype(BF16)

    pick_place = selector(0)
    pick_high = selector(experts)
    pick_low = selector(2 * experts)
    slot_rank = (lax.broadcasted_iota(jnp.int32, (slots, local_tokens), 0) % cap + 1).astype(F32)
    slot_of_lane = (lax.broadcasted_iota(jnp.int32, (local_tokens, slots), 1) % cap + 1).astype(F32)
    peers = [lax.rem(p + e, inner) for e in range(1, inner)]

    def half_of(which):
        return pl.ds(pl.multiple_of(which * half, half), half)

    def dispatch(i):
        j = order[i]
        if i:
            arrive(column.at[j], col_send.at[j], col_recv.at[j])
            on, wanted = passes(j)

            @pl.when(wanted)
            def _():
                column_copy(j, on, col_pass.at[j]).start()

        where = dot_t(pick_place, column[j, :, half:])
        onehot = jnp.where(where == slot_rank, 1.0, 0.0).astype(BF16)
        moved = dot(onehot, column[j, :, :half]).astype(BF16)
        staged[j] = moved.reshape(inner, cap, half)
        for to in peers:
            send(
                staged.at[j, to],
                rows_in.at[tp, j, p],
                plane_send.at[j, to],
                plane_recv.at[j, p],
                z * inner + to,
                tp,
            )
        rows_in[tp, j, p] = staged[j, p]

    def pair(i):
        j = order[i]
        for source in peers:
            arrive(rows_in.at[tp, j, source], plane_send.at[j, source], plane_recv.at[j, source])
        here = rows_in.at[tp, j]
        send(here, here, pair_send.at[j], pair_recv.at[j], ep, other)

    def expert(group):
        if group[0] == 0:
            for load in loads[3:]:
                load.wait()

        def rows_of(which):
            blocks = [rows_in[which, order[i]].reshape(slots, half) for i in group]
            return jnp.concatenate(blocks, axis=0)

        own_rows = rows_of(tp)
        gate_value = dot(own_rows, gate_w[half_of(tp), :])
        upward = dot(own_rows, up_w[half_of(tp), :])
        for i in group:
            j = order[i]
            arrive(rows_in.at[other, j], pair_send.at[j], pair_recv.at[j])
        other_rows = rows_of(other)
        gate_value = gate_value + dot(other_rows, gate_w[half_of(other), :])
        upward = upward + dot(other_rows, up_w[half_of(other), :])
        hidden = silu_product(gate_value, upward)

        def store(target, values):
            for n, i in enumerate(group):
                block = values[n * slots : (n + 1) * slots]
                target[order[i]] = block.astype(BF16).reshape(inner, cap, half)

        store(part_out, dot(hidden, down_w[:, half_of(other)]))
        for i in reversed(group):
            j = order[i]
            send(part_out.at[j], part_in.at[j], part_send.at[j], part_recv.at[j], ep, other)
        store(part_own, dot(hidden, down_w[:, half_of(tp)]))

    def give_back(i):
        j = order[i]
        arrive(part_in.at[j], part_send.at[j], part_recv.at[j])
        result[j] = (part_own[j].astype(F32) + part_in[j].astype(F32)).astype(BF16)
        for to in peers:
            send(
                result.at[j, to],
                back.at[j, p],
                back_send.at[j, to],
                back_recv.at[j, p],
                z * inner + to,
                tp,
            )
        back[j, p] = result[j, p]

    def combine(i):
        j = order[i]
        facts = column[j, :, half:]
        chosen = dot_t(facts, pick_place) == slot_of_lane
        high_part = jnp.where(chosen, dot_t(facts, pick_high), 0.0).astype(BF16)
        low_part = jnp.where(chosen, dot_t(facts, pick_low), 0.0).astype(BF16)
        for source in peers:
            arrive(back.at[j, source], back_send.at[j, source], back_recv.at[j, source])
        values = back[j].reshape(slots, half)
        return dot(high_part, values) + dot(low_part, values)

    dispatch(0)

    for load in loads[:3]:
        load.wait()
    inputs = normed[...]
    shared_hidden = silu_product(dot(inputs, sgate_w[...]), dot(inputs, sup_w[...]))
    shared_out[...] = dot(shared_hidden, sdown_w[:, half_of(other)]).astype(BF16)
    send(shared_out, shared_in, shared_sem.at[0], shared_sem.at[1], ep, other)
    shared_own = dot(shared_hidden, sdown_w[:, half_of(tp)]).astype(BF16)

    def step(task, what):
        with jax.named_scope(task.__name__ + str(what)):
            task(what)

    paired = 0
    for i in range(1, outer):
        step(dispatch, i)
        if i < outer - 1:
            step(pair, paired)
            paired += 1
    for group in [[i, i + 1] for i in range(0, outer, 2)]:
        while paired <= group[-1]:
            step(pair, paired)
            paired += 1
        step(expert, group)
        for i in reversed(group):
            step(give_back, i)

    for i in [1] + list(range(outer - 1, 1, -1)):
        j = order[i]
        with jax.named_scope("combine" + str(i)):
            sum_out[j] = combine(i).astype(BF16)
            send(sum_out.at[j], sum_in.at[z], sum_send.at[j], sum_recv.at[z], j * inner + p, tp)
    with jax.named_scope("combine0"):
        combined = combine(0)
        arrive(shared_in, shared_sem.at[0], shared_sem.at[1])
        shared_rows = (shared_own.astype(F32) + shared_in[...].astype(F32)).astype(BF16)
        combined = combined + shared_rows.astype(F32)
    for j in order[1:]:
        arrive(sum_in.at[j], sum_send.at[j], sum_recv.at[j])
        combined = combined + sum_in[j].astype(F32)

    own_squares = jnp.sum(combined * combined, axis=1, keepdims=True)
    squares_out[...] = jnp.broadcast_to(own_squares, squares_out.shape)
    sq_copy = remote(squares_out, squares_in, sq_sem.at[0], sq_sem.at[1], ep, other)
    sq_copy.start()
    sq_copy.wait_recv()
    squares = own_squares + squares_in[:, :1]
    scaled = combined * lax.rsqrt(squares / width + EPSILON)
    mixed[...] = (scaled * out_gain[...].astype(F32)[None, :]).astype(BF16)

    for to in order[1:]:

        @pl.when(direct(to))
        def _(to=to):
            column_copy(z, to, col_send.at[to]).wait_send()

        on, wanted = passes(to)

        @pl.when(wanted)
        def _(to=to, on=on):
            column_copy(to, on, col_pass.at[to]).wait_send()

    for copy in sends:
        copy.wait_send()
    sq_copy.wait_send()


def body(
    experts,
    tokens,
    in_gain,
    route_expert,
    route_weight,
    gate_weight,
    up_weight,
    down_weight,
    shared_gate,
    shared_up,
    shared_down,
    out_gain,
):
    inner = 1
    while inner * inner < experts:
        inner *= 2
    outer = experts // inner
    local_tokens, width = tokens.shape
    half = width // 2
    top_count = route_expert.shape[1]
    capacity = max(2, (local_tokens * top_count * 4 + 3 * experts - 1) // (3 * experts))
    cap = -(-capacity // 16) * 16
    info_width = -(-3 * experts // 128) * 128
    hidden = gate_weight.shape[2]
    shared_width = shared_gate.shape[1]

    def vm(shape, kind=BF16):
        return pltpu.VMEM(shape, kind)

    grid_rows = (outer, inner, cap, half)
    dma = pltpu.SemaphoreType.DMA
    in_vmem = pl.BlockSpec(memory_space=pltpu.VMEM)
    anywhere = pl.BlockSpec(memory_space=pl.ANY)
    return pl.pallas_call(
        functools.partial(kernel, outer, inner, cap, info_width),
        out_shape=jax.ShapeDtypeStruct((local_tokens, half), BF16),
        in_specs=[in_vmem] * 5 + [anywhere] * 6,
        out_specs=in_vmem,
        scratch_shapes=[
            vm((width, hidden)),
            vm((width, hidden)),
            vm((hidden, width)),
            vm((width, shared_width)),
            vm((width, shared_width)),
            vm((shared_width, width)),
            vm((local_tokens, width)),
            vm((outer, local_tokens, half + info_width)),
            vm(grid_rows),
            vm((2,) + grid_rows),
            vm(grid_rows),
            vm(grid_rows),
            vm(grid_rows),
            vm(grid_rows),
            vm(grid_rows),
            vm((outer, local_tokens, half)),
            vm((outer, local_tokens, half)),
            vm((local_tokens, half)),
            vm((local_tokens, half)),
            vm((local_tokens, 128), F32),
            vm((local_tokens, 128), F32),
            dma((6,)),
            dma((outer,)),
            dma((outer,)),
            dma((outer,)),
            dma((outer, inner)),
            dma((outer, inner)),
            dma((outer,)),
            dma((outer,)),
            dma((outer,)),
            dma((outer,)),
            dma((2,)),
            dma((outer, inner)),
            dma((outer, inner)),
            dma((outer,)),
            dma((outer,)),
            dma((2,)),
        ],
        compiler_params=pltpu.CompilerParams(
            collective_id=0, has_side_effects=True, vmem_limit_bytes=60 * 1024 * 1024
        ),
    )(
        tokens,
        in_gain,
        route_expert.T,
        route_weight.T,
        out_gain,
        gate_weight,
        up_weight,
        down_weight,
        shared_gate,
        shared_up,
        shared_down,
    )


def solution(mesh):
    return jax.shard_map(
        functools.partial(body, mesh.shape["ep"]),
        mesh=mesh,
        in_specs=(
            P(("grp", "ep"), None),
            P(),
            P(("grp", "ep"), None),
            P(("grp", "ep"), None),
            P("ep", None, "tp"),
            P("ep", None, "tp"),
            P("ep", "tp", None),
            P(None, "tp"),
            P(None, "tp"),
            P("tp", None),
            P("tp"),
        ),
        out_specs=P(("grp", "ep"), "tp"),
        check_vma=False,
    )
```

```python
import functools

import jax
import jax.numpy as jnp
from jax import lax
from jax.experimental import pallas as pl
from jax.experimental.pallas import tpu as pltpu
from jax.sharding import PartitionSpec as P

EPSILON = 1e-06
F32 = jnp.float32
BF16 = jnp.bfloat16


def dot(a, b):
    return jnp.dot(a, b, preferred_element_type=F32)


def dot_t(a, b):
    return lax.dot_general(a, b, (((1,), (1,)), ((), ())), preferred_element_type=F32)


def silu_product(gate_value, upward):
    return (gate_value * (1.0 / (1.0 + jnp.exp(-gate_value))) * upward).astype(BF16)


def kernel(
    outer,
    inner,
    cap,
    info_width,
    tokens_hbm,
    in_gain_hbm,
    route_expert_hbm,
    route_weight_hbm,
    out_gain_hbm,
    gate_hbm,
    up_hbm,
    down_hbm,
    sgate_hbm,
    sup_hbm,
    sdown_hbm,
    mixed,
    tokens,
    in_gain,
    route_expert,
    route_weight,
    out_gain,
    gate_w,
    up_w,
    down_w,
    sgate_w,
    sup_w,
    sdown_w,
    normed,
    column,
    staged,
    rows_in,
    part_out,
    part_in,
    part_own,
    result,
    back,
    sum_out,
    sum_in,
    shared_out,
    shared_in,
    squares_out,
    squares_in,
    w_sem,
    col_send,
    col_recv,
    col_pass,
    plane_send,
    plane_recv,
    pair_send,
    pair_recv,
    part_send,
    part_recv,
    shared_sem,
    back_send,
    back_recv,
    sum_send,
    sum_recv,
    sq_sem,
):
    ep = lax.axis_index("ep")
    tp = lax.axis_index("tp")
    z = ep // inner
    p = ep % inner
    other = 1 - tp
    experts = outer * inner
    local_tokens, width = tokens.shape
    half = width // 2

    loads = [
        pltpu.make_async_copy(src, dst, w_sem.at[i])
        for i, (src, dst) in enumerate(
            [
                (tokens_hbm, tokens),
                (in_gain_hbm, in_gain),
                (route_expert_hbm, route_expert),
                (route_weight_hbm, route_weight),
                (out_gain_hbm, out_gain),
                (sgate_hbm, sgate_w),
                (sup_hbm, sup_w),
                (sdown_hbm, sdown_w),
                (gate_hbm.at[0], gate_w),
                (up_hbm.at[0], up_w),
                (down_hbm.at[0], down_w),
            ]
        )
    ]
    for load in loads[:5]:
        load.start()

    barrier = pltpu.get_barrier_semaphore()

    def greet(ep_to, tp_to):
        pl.semaphore_signal(
            barrier, inc=1, device_id={"ep": ep_to, "tp": tp_to}, device_id_type=pl.DeviceIdType.MESH
        )

    for d in range(1, outer):
        greet(lax.rem(z + d, outer) * inner + p, tp)
    for d in range(1, inner):
        greet(z * inner + lax.rem(p + d, inner), tp)
    greet(ep, other)

    def remote(src, dst, send, recv, ep_to, tp_to):
        return pltpu.make_async_remote_copy(
            src_ref=src,
            dst_ref=dst,
            send_sem=send,
            recv_sem=recv,
            device_id={"ep": ep_to, "tp": tp_to},
            device_id_type=pl.DeviceIdType.MESH,
        )

    for load in loads[:5]:
        load.wait()
    for load in loads[5:]:
        load.start()
    floats = tokens[...].astype(F32)
    mean = jnp.sum(floats * floats, axis=1, keepdims=True) / width
    rows = (floats * lax.rsqrt(mean + EPSILON) * in_gain[...].astype(F32)[None, :]).astype(BF16)
    normed[...] = rows

    fact = lax.broadcasted_iota(jnp.int32, (info_width, local_tokens), 0)
    fact_expert = lax.rem(fact, experts)
    named = jnp.zeros((info_width, local_tokens), F32)
    weight = jnp.zeros((info_width, local_tokens), F32)
    for k in range(route_expert.shape[0]):
        hit = route_expert[k : k + 1, :] == fact_expert
        named = named + jnp.where(hit, 1.0, 0.0)
        weight = weight + jnp.where(hit, route_weight[k : k + 1, :], 0.0)
    row_i = lax.broadcasted_iota(jnp.int32, (local_tokens, local_tokens), 0)
    col_i = lax.broadcasted_iota(jnp.int32, (local_tokens, local_tokens), 1)
    upto = jnp.where(row_i <= col_i, 1.0, 0.0).astype(BF16)
    place = dot(named.astype(BF16), upto) * named
    high = weight.astype(BF16).astype(F32)
    facts = jnp.where(fact < experts, place, jnp.where(fact < 2 * experts, high, weight - high))
    facts = jnp.where(fact < 3 * experts, facts, 0.0).astype(BF16)
    same = jnp.where(row_i == col_i, 1.0, 0.0).astype(BF16)
    info = dot_t(same, facts)

    @pl.when(tp == 0)
    def _():
        column[z, :, :half] = rows[:, :half]

    @pl.when(tp == 1)
    def _():
        column[z, :, :half] = rows[:, half:]

    column[z, :, half:] = info.astype(BF16)

    pl.semaphore_wait(barrier, outer + inner - 1)

    sends = []

    def send(src, dst, send_sem, recv_sem, ep_to, tp_to):
        copy = remote(src, dst, send_sem, recv_sem, ep_to, tp_to)
        copy.start()
        sends.append(copy)

    def arrive(ref, send_sem, recv_sem):
        remote(ref, ref, send_sem, recv_sem, ep, other).wait_recv()

    short = jnp.minimum(z, outer - 1 - z)

    def nth(i):
        if i == 0:
            return z
        near = (i + 1) // 2 if i % 2 else -(i // 2)
        far = jnp.where(z < outer - 1 - z, i - short, short - i)
        return z + jnp.where(i <= 2 * short, near, far)

    order = [nth(i) for i in range(outer)]

    def column_copy(block, to, send_sem):
        here = column.at[block]
        return remote(here, here, send_sem, col_recv.at[block], to * inner + p, tp)

    def direct(to):
        return (to - z) * (to - z) != 4

    def passes(j):
        on = 2 * z - j
        return on, ((j - z) * (j - z) == 1) & (on >= 0) & (on < outer)

    for to in order[1:]:

        @pl.when(direct(to))
        def _(to=to):
            column_copy(z, to, col_send.at[to]).start()


    slots = inner * cap
    slot_row = lax.broadcasted_iota(jnp.int32, (slots, info_width), 0)
    slot_lane = lax.broadcasted_iota(jnp.int32, (slots, info_width), 1)
    slot_expert = z * inner + slot_row // cap

    def selector(offset):
        return jnp.where(slot_lane == slot_expert + offset, 1.0, 0.0).astype(BF16)

    pick_place = selector(0)
    pick_high = selector(experts)
    pick_low = selector(2 * experts)
    slot_rank = (lax.broadcasted_iota(jnp.int32, (slots, local_tokens), 0) % cap + 1).astype(F32)
    slot_of_lane = (lax.broadcasted_iota(jnp.int32, (local_tokens, slots), 1) % cap + 1).astype(F32)
    peers = [lax.rem(p + e, inner) for e in range(1, inner)]

    def half_of(which):
        return pl.ds(pl.multiple_of(which * half, half), half)

    def dispatch(i):
        j = order[i]
        if i:
            arrive(column.at[j], col_send.at[j], col_recv.at[j])
            on, wanted = passes(j)

            @pl.when(wanted)
            def _():
                column_copy(j, on, col_pass.at[j]).start()

        where = dot_t(pick_place, column[j, :, half:])
        onehot = jnp.where(where == slot_rank, 1.0, 0.0).astype(BF16)
        moved = dot(onehot, column[j, :, :half]).astype(BF16)
        staged[j] = moved.reshape(inner, cap, half)
        for to in peers:
            send(
                staged.at[j, to],
                rows_in.at[tp, j, p],
                plane_send.at[j, to],
                plane_recv.at[j, p],
                z * inner + to,
                tp,
            )
        rows_in[tp, j, p] = staged[j, p]

    def pair(i):
        j = order[i]
        for source in peers:
            arrive(rows_in.at[tp, j, source], plane_send.at[j, source], plane_recv.at[j, source])
        here = rows_in.at[tp, j]
        send(here, here, pair_send.at[j], pair_recv.at[j], ep, other)

    def expert(group):
        if group[0] == 0:
            for load in loads[8:]:
                load.wait()

        def rows_of(which):
            blocks = [rows_in[which, order[i]].reshape(slots, half) for i in group]
            return jnp.concatenate(blocks, axis=0)

        own_rows = rows_of(tp)
        gate_value = dot(own_rows, gate_w[half_of(tp), :])
        upward = dot(own_rows, up_w[half_of(tp), :])
        for i in group:
            j = order[i]
            arrive(rows_in.at[other, j], pair_send.at[j], pair_recv.at[j])
        other_rows = rows_of(other)
        gate_value = gate_value + dot(other_rows, gate_w[half_of(other), :])
        upward = upward + dot(other_rows, up_w[half_of(other), :])
        hidden = silu_product(gate_value, upward)

        def store(target, values):
            for n, i in enumerate(group):
                block = values[n * slots : (n + 1) * slots]
                target[order[i]] = block.astype(BF16).reshape(inner, cap, half)

        store(part_out, dot(hidden, down_w[:, half_of(other)]))
        for i in reversed(group):
            j = order[i]
            send(part_out.at[j], part_in.at[j], part_send.at[j], part_recv.at[j], ep, other)
        store(part_own, dot(hidden, down_w[:, half_of(tp)]))

    def give_back(i):
        j = order[i]
        arrive(part_in.at[j], part_send.at[j], part_recv.at[j])
        result[j] = (part_own[j].astype(F32) + part_in[j].astype(F32)).astype(BF16)
        for to in peers:
            send(
                result.at[j, to],
                back.at[j, p],
                back_send.at[j, to],
                back_recv.at[j, p],
                z * inner + to,
                tp,
            )
        back[j, p] = result[j, p]

    def combine(i):
        j = order[i]
        facts = column[j, :, half:]
        chosen = dot_t(facts, pick_place) == slot_of_lane
        high_part = jnp.where(chosen, dot_t(facts, pick_high), 0.0).astype(BF16)
        low_part = jnp.where(chosen, dot_t(facts, pick_low), 0.0).astype(BF16)
        for source in peers:
            arrive(back.at[j, source], back_send.at[j, source], back_recv.at[j, source])
        values = back[j].reshape(slots, half)
        return dot(high_part, values) + dot(low_part, values)

    dispatch(0)

    for load in loads[5:8]:
        load.wait()
    inputs = normed[...]
    shared_hidden = silu_product(dot(inputs, sgate_w[...]), dot(inputs, sup_w[...]))
    shared_out[...] = dot(shared_hidden, sdown_w[:, half_of(other)]).astype(BF16)
    send(shared_out, shared_in, shared_sem.at[0], shared_sem.at[1], ep, other)
    shared_own = dot(shared_hidden, sdown_w[:, half_of(tp)]).astype(BF16)

    def step(task, what):
        with jax.named_scope(task.__name__ + str(what)):
            task(what)

    for i in range(1, outer):
        step(dispatch, i)
        if i == 1:
            step(pair, 0)
    step(pair, 1)
    for first in range(0, outer, 2):
        step(expert, (first, first + 1))
        if first + 2 < outer:
            step(pair, first + 2)
            step(pair, first + 3)
        step(give_back, first + 1)
        step(give_back, first)

    for i in [1] + list(range(outer - 1, 1, -1)):
        j = order[i]
        with jax.named_scope("combine" + str(i)):
            sum_out[j] = combine(i).astype(BF16)
            send(sum_out.at[j], sum_in.at[z], sum_send.at[j], sum_recv.at[z], j * inner + p, tp)
    with jax.named_scope("combine0"):
        combined = combine(0)
        arrive(shared_in, shared_sem.at[0], shared_sem.at[1])
        shared_rows = (shared_own.astype(F32) + shared_in[...].astype(F32)).astype(BF16)
        combined = combined + shared_rows.astype(F32)
    for j in order[1:]:
        arrive(sum_in.at[j], sum_send.at[j], sum_recv.at[j])
        combined = combined + sum_in[j].astype(F32)

    own_squares = jnp.sum(combined * combined, axis=1, keepdims=True)
    squares_out[...] = jnp.broadcast_to(own_squares, squares_out.shape)
    sq_copy = remote(squares_out, squares_in, sq_sem.at[0], sq_sem.at[1], ep, other)
    sq_copy.start()
    sq_copy.wait_recv()
    squares = own_squares + squares_in[:, :1]
    scaled = combined * lax.rsqrt(squares / width + EPSILON)
    mixed[...] = (scaled * out_gain[...].astype(F32)[None, :]).astype(BF16)

    for to in order[1:]:

        @pl.when(direct(to))
        def _(to=to):
            column_copy(z, to, col_send.at[to]).wait_send()

        on, wanted = passes(to)

        @pl.when(wanted)
        def _(to=to, on=on):
            column_copy(to, on, col_pass.at[to]).wait_send()

    for copy in sends:
        copy.wait_send()
    sq_copy.wait_send()


def body(
    experts,
    tokens,
    in_gain,
    route_expert,
    route_weight,
    gate_weight,
    up_weight,
    down_weight,
    shared_gate,
    shared_up,
    shared_down,
    out_gain,
):
    inner = 1
    while inner * inner < experts:
        inner *= 2
    outer = experts // inner
    local_tokens, width = tokens.shape
    half = width // 2
    top_count = route_expert.shape[1]
    capacity = max(2, (local_tokens * top_count * 4 + 3 * experts - 1) // (3 * experts))
    cap = -(-capacity // 16) * 16
    info_width = -(-3 * experts // 128) * 128
    hidden = gate_weight.shape[2]
    shared_width = shared_gate.shape[1]

    def vm(shape, kind=BF16):
        return pltpu.VMEM(shape, kind)

    grid_rows = (outer, inner, cap, half)
    dma = pltpu.SemaphoreType.DMA
    in_vmem = pl.BlockSpec(memory_space=pltpu.VMEM)
    anywhere = pl.BlockSpec(memory_space=pl.ANY)
    return pl.pallas_call(
        functools.partial(kernel, outer, inner, cap, info_width),
        out_shape=jax.ShapeDtypeStruct((local_tokens, half), BF16),
        in_specs=[anywhere] * 11,
        out_specs=in_vmem,
        scratch_shapes=[
            vm((local_tokens, width)),
            vm((width,)),
            vm((top_count, local_tokens), jnp.int32),
            vm((top_count, local_tokens), F32),
            vm((half,)),
            vm((width, hidden)),
            vm((width, hidden)),
            vm((hidden, width)),
            vm((width, shared_width)),
            vm((width, shared_width)),
            vm((shared_width, width)),
            vm((local_tokens, width)),
            vm((outer, local_tokens, half + info_width)),
            vm(grid_rows),
            vm((2,) + grid_rows),
            vm(grid_rows),
            vm(grid_rows),
            vm(grid_rows),
            vm(grid_rows),
            vm(grid_rows),
            vm((outer, local_tokens, half)),
            vm((outer, local_tokens, half)),
            vm((local_tokens, half)),
            vm((local_tokens, half)),
            vm((local_tokens, 128), F32),
            vm((local_tokens, 128), F32),
            dma((11,)),
            dma((outer,)),
            dma((outer,)),
            dma((outer,)),
            dma((outer, inner)),
            dma((outer, inner)),
            dma((outer,)),
            dma((outer,)),
            dma((outer,)),
            dma((outer,)),
            dma((2,)),
            dma((outer, inner)),
            dma((outer, inner)),
            dma((outer,)),
            dma((outer,)),
            dma((2,)),
        ],
        compiler_params=pltpu.CompilerParams(
            collective_id=0, has_side_effects=True, vmem_limit_bytes=60 * 1024 * 1024
        ),
    )(
        tokens,
        in_gain,
        route_expert.T,
        route_weight.T,
        out_gain,
        gate_weight,
        up_weight,
        down_weight,
        shared_gate,
        shared_up,
        shared_down,
    )


def solution(mesh):
    return jax.shard_map(
        functools.partial(body, mesh.shape["ep"]),
        mesh=mesh,
        in_specs=(
            P(("grp", "ep"), None),
            P(),
            P(("grp", "ep"), None),
            P(("grp", "ep"), None),
            P("ep", None, "tp"),
            P("ep", None, "tp"),
            P("ep", "tp", None),
            P(None, "tp"),
            P(None, "tp"),
            P("tp", None),
            P("tp"),
        ),
        out_specs=P(("grp", "ep"), "tp"),
        check_vma=False,
    )
```
